256 devices in a mesh: grp: 2 (over z), fs: 16 (over y, core), tp: 8 (over x).
Axes of the slice: x: 8, y: 8, z: 2, core: 2. Of those that a mesh axis runs over, the one named last changes fastest.
The devices are a block of a 8x8x16 slice.
Arguments:
- prompt_tokens: bfloat16 [32768, 2048], P(('grp', 'fs', 'tp')), parts along dimension 0, may hold values from -6 to 6
- up_weight: float32 [2048, 8192], P('fs', 'tp'), may hold values from -0.125 to 0.125
- down_weight: float32 [2048, 8192], P('fs', 'tp'), may hold values from -0.0625 to 0.0625
- pre_gain: float32 [2048], P('fs'), may hold values from 0.1 to 1.9
- post_gain: float32 [2048], replicated, may hold values from 0.1 to 1.9
Outputs:
- mixed: bfloat16 [32768, 2048], P(('grp', 'fs', 'tp')), parts along dimension 0
- sampler_up: bfloat16 [4096, 8192], P('grp', 'tp'), parts along dimension 0
- sampler_down: bfloat16 [4096, 8192], P('grp', 'tp'), parts along dimension 0
The draws below stay inside these ranges and needn't reach their ends.
There are 2 independent parts, one for each index of `grp`. The reference program is written for one: setup_inputs(seed, part) draws one part's arguments, and reference() takes and returns one part's arrays. A program takes and returns all parts, laid end to end along the dimension named above; an argument that names none is the same for every part. Nothing has to cross between parts.
All inputs are finite; a program needn't handle non-finite values.
Results may differ from the reference program's by a relative error of at most 0.015.
Values may be sent and summed in bfloat16 or wider, within the bound.
A program may use at most 128 MiB of HBM per device.

```python
import jax
import jax.numpy as jnp
from jax import lax

D = 2048
FF = 8192
TOK_DEV = 128
TOKENS = 16384
N_TP = 8


def shard_levels(stream_key, extent, split, low, top_value):
    loudness = 1.0
    for dim, blocks in split:
        heights = jax.random.uniform(jax.random.fold_in(jax.random.fold_in(stream_key, 6), dim), (blocks,), jnp.float32, low / len(split), top_value / len(split))
        loudness = loudness * jnp.repeat(jnp.exp(heights), extent[dim] // blocks).reshape((-1,) + (1,) * (len(extent) - 1 - dim))
    return loudness


def gaussian(key, shape, scale, reach, shards=(), dtype=jnp.bfloat16):
    values = jax.random.normal(key, shape, jnp.float32) * scale
    if len(shards) > 0:
        values = shard_levels(key, shape, shards, -0.22, 0.18) * values
    return jnp.clip(values, min=-reach, max=reach).astype(dtype)


def setup_inputs(seed: int = 0, part: int = 0) -> dict:
    arg_keys = jax.random.split(jax.random.key(seed), 6)
    part_splits = jax.random.split(jax.random.fold_in(arg_keys[5], part), 6)
    return {
        "prompt_tokens": gaussian(part_splits[0], (TOKENS, D), 1.0, 6.0, ((0, 128),)),
        "up_weight": gaussian(arg_keys[1], (D, FF), D ** -0.5, 0.125, ((0, 16), (1, 8)), jnp.float32),
        "down_weight": gaussian(arg_keys[2], (D, FF), FF ** -0.5, 0.0625, ((0, 16), (1, 8)), jnp.float32),
        "pre_gain": jnp.clip(1.0 + 0.18 * jax.random.normal(arg_keys[3], (D,), jnp.float32), 0.1, 1.9),
        "post_gain": jnp.clip(1.0 + 0.18 * jax.random.normal(arg_keys[4], (D,), jnp.float32), 0.1, 1.9),
    }


def reference(prompt_tokens, up_weight, down_weight, pre_gain, post_gain):
    sampler_up = (up_weight * pre_gain[:, None]).astype(jnp.bfloat16)
    sampler_down = down_weight.astype(jnp.bfloat16)
    width = prompt_tokens.shape[1]
    hidden_units = up_weight.shape[1]
    block_rows = TOK_DEV * N_TP
    blocks = prompt_tokens.reshape(TOKENS // block_rows, block_rows, width)
    down_split = sampler_down.astype(jnp.float32).reshape(width, N_TP, hidden_units // N_TP)

    def one_block(rows):
        values = rows.astype(jnp.float32)
        normed = (values * lax.rsqrt(lax.optimization_barrier(jnp.mean(values * values, axis=1, keepdims=True)) + 1e-06)).astype(jnp.bfloat16)
        lifted = jnp.dot(normed, sampler_up, preferred_element_type=jnp.float32)
        hidden = jnp.square(jax.nn.relu(lifted)).astype(jnp.bfloat16)
        hidden_split = hidden.astype(jnp.float32).reshape(block_rows, N_TP, hidden_units // N_TP)
        parts = jnp.einsum('rbk,dbk->brd', hidden_split, down_split).astype(jnp.bfloat16)
        summed = lax.optimization_barrier(jnp.sum(parts.astype(jnp.float32), axis=0))
        scaled = summed * lax.rsqrt(lax.optimization_barrier(jnp.mean(summed * summed, axis=1, keepdims=True)) + 1e-06)
        return (scaled * post_gain[None, :]).astype(jnp.bfloat16)
    mixed = lax.map(one_block, blocks).reshape(TOKENS, width)
    return (mixed, sampler_up, sampler_down)
```

```python
import functools

import jax
import jax.numpy as jnp
from jax import lax
from jax.experimental import pallas as pl
from jax.experimental.pallas import tpu as pltpu
from jax.sharding import PartitionSpec as P

MESH = pl.DeviceIdType.MESH
EPS = 1e-06
TILE = 256


def ring_items(n):
    far = n // 2
    return [(k % 2, k // 2) for k in range(2 * far - 1)]


def kernel(
    n_tp,
    n_fs,
    tok_hbm,
    up_hbm,
    down_hbm,
    pre_ref,
    post_ref,
    mixed_ref,
    wu,
    wd,
    tok_in,
    up_in,
    down_in,
    tok,
    hid,
    part,
    outbox,
    inbox,
    in_sem,
    x_send,
    x_recv,
    y_send,
    y_recv,
    c_send,
    c_recv,
    r_send,
    r_recv,
):
    t = lax.axis_index("tp")
    f = lax.axis_index("fs")
    x_peer = ({"tp": lax.rem(t + 1, n_tp)}, {"tp": lax.rem(t + n_tp - 1, n_tp)})
    y_peer = ({"fs": lax.rem(f + 2, n_fs)}, {"fs": lax.rem(f + n_fs - 2, n_fs)})
    core_peer = {"fs": f + 1 - 2 * lax.rem(f, 2)}
    rows, width = tok_in.shape
    shard = up_in.shape[0]
    half = rows // 2
    wide = width // 2
    n_pairs = n_tp // 2

    barrier = pltpu.get_barrier_semaphore()
    for peer in (*x_peer, *y_peer, core_peer):
        pl.semaphore_signal(barrier, inc=1, device_id=peer, device_id_type=MESH)
    loads = [
        pltpu.make_async_copy(src, dst, in_sem.at[k])
        for k, (src, dst) in enumerate(((up_hbm, up_in), (down_hbm, down_in), (tok_hbm, tok_in)))
    ]
    for load in loads:
        load.start()

    def shard_rows(index):
        return pl.ds(pl.multiple_of(index * shard, shard), shard)

    loads[0].wait()
    gain = jnp.broadcast_to(pre_ref[...], (shard, shard)).T
    for c in range(up_in.shape[1] // shard):
        cols = pl.ds(c * shard, shard)
        wu[shard_rows(f), cols] = (up_in[:, cols] * gain).astype(jnp.bfloat16)
    loads[1].wait()
    wd[shard_rows(f), :] = down_in[...].astype(jnp.bfloat16)
    loads[2].wait()
    values = tok_in[...].astype(jnp.float32)
    scale = lax.rsqrt(jnp.mean(values * values, axis=1, keepdims=True) + EPS)
    tok[0, rows:, :] = (values * scale).astype(jnp.bfloat16)

    pl.semaphore_wait(barrier, 5)

    def tok_slot(direction, distance):
        if distance == 0:
            return 0, rows
        if distance == n_pairs:
            return 0, 0
        return distance, (rows if direction == 0 else 0)

    def tok_piece(direction, which, distance):
        pair, row = tok_slot(direction, distance)
        return tok.at[pair, pl.ds(row + which * half, half), :]

    def weight_piece(direction, which, distance):
        step = 2 * distance
        owner = lax.rem(f + n_fs - step, n_fs) if direction == 0 else lax.rem(f + step, n_fs)
        return (wu, wd)[which].at[shard_rows(owner), :]

    def x_copy(direction, k):
        which, distance = ring_items(n_tp)[k]
        which = which if direction == 0 else 1 - which
        return pltpu.make_async_remote_copy(
            src_ref=tok_piece(direction, which, distance),
            dst_ref=tok_piece(direction, which, distance + 1),
            send_sem=x_send.at[direction, k],
            recv_sem=x_recv.at[direction, k],
            device_id=x_peer[direction],
            device_id_type=MESH,
        )

    def y_copy(direction, k):
        which, distance = ring_items(n_fs // 2)[k]
        which = which if direction == 0 else 1 - which
        piece = weight_piece(direction, which, distance)
        return pltpu.make_async_remote_copy(
            src_ref=piece,
            dst_ref=piece,
            send_sem=y_send.at[direction, k],
            recv_sem=y_recv.at[direction, k],
            device_id=y_peer[direction],
            device_id_type=MESH,
        )

    def core_copy(slot, piece):
        return pltpu.make_async_remote_copy(
            src_ref=piece,
            dst_ref=piece,
            send_sem=c_send.at[slot],
            recv_sem=c_recv.at[slot],
            device_id=core_peer,
            device_id_type=MESH,
        )

    x_steps = len(ring_items(n_tp))
    y_steps = len(ring_items(n_fs // 2))
    xs = [[x_copy(d, k) for k in range(x_steps)] for d in range(2)]
    ys = [[y_copy(d, k) for k in range(y_steps)] for d in range(2)]
    cs = []
    for k in range(2):
        for d in range(2):
            ys[d][k].start()
        for d in range(2):
            xs[d][k].start()
    for which in range(2):
        cs.append(core_copy(which, weight_piece(0, which, 0)))
        cs[-1].start()
    for k in range(max(x_steps, y_steps)):
        for d in range(2):
            if k < y_steps:
                ys[d][k].wait_recv()
                if k + 2 < y_steps:
                    ys[d][k + 2].start()
                which, distance = ring_items(n_fs // 2)[k]
                which = which if d == 0 else 1 - which
                cs.append(core_copy(2 + d * y_steps + k, weight_piece(d, which, distance + 1)))
                cs[-1].start()
        for d in range(2):
            if k < x_steps:
                xs[d][k].wait_recv()
                if k + 2 < x_steps:
                    xs[d][k + 2].start()
    for copy in cs:
        copy.wait_recv()

    def hidden(pair):
        def one(n, carry):
            cols = pl.ds(pl.multiple_of(n * TILE, TILE), TILE)
            lifted = jnp.dot(tok[pair], wu[:, cols], preferred_element_type=jnp.float32)
            lifted = jnp.maximum(lifted, 0.0)
            hid[pair, :, cols] = (lifted * lifted).astype(jnp.bfloat16)
            return carry

        lax.fori_loop(0, hid.shape[2] // TILE, one, 0)

    def partial(pair, which):
        def one(n, carry):
            cols = pl.ds(pl.multiple_of(which * wide + n * TILE, TILE), TILE)
            part[pair, :, cols] = lax.dot_general(
                hid[pair],
                wd[cols, :],
                (((1,), (1,)), ((), ())),
                preferred_element_type=jnp.float32,
            )
            return carry

        lax.fori_loop(0, wide // TILE, one, 0)

    def r_copy(direction, k):
        return pltpu.make_async_remote_copy(
            src_ref=outbox.at[direction, k],
            dst_ref=inbox.at[direction, k],
            send_sem=r_send.at[direction, k],
            recv_sem=r_recv.at[direction, k],
            device_id=x_peer[direction],
            device_id_type=MESH,
        )

    rs = [[r_copy(d, k) for k in range(x_steps)] for d in range(2)]

    def pass_on(k, directions=(0, 1)):
        for d in directions:
            which, travelled = ring_items(n_tp)[x_steps - 1 - k]
            which = which if d == 0 else 1 - which
            ahead = travelled + 1
            pair, row = (0, 0) if ahead == n_pairs else (ahead, 0 if d == 0 else rows)
            own = part[pair, pl.ds(row, rows), pl.ds(which * wide, wide)]
            if k >= 2:
                rs[d][k - 2].wait_recv()
                own = own + inbox[d, k - 2].astype(jnp.float32)
            outbox[d, k] = own.astype(jnp.bfloat16)
        for d in directions:
            rs[d][k].start()

    hidden(0)
    partial(0, 0)
    pass_on(0, (0,))
    partial(0, 1)
    pass_on(0, (1,))
    for pair in range(n_pairs - 1, 0, -1):
        hidden(pair)
        partial(pair, 0)
        partial(pair, 1)
        first = 2 * (n_pairs - 1 - pair) + 1
        pass_on(first)
        pass_on(first + 1)

    last = x_steps - 1
    halves = []
    for which in range(2):
        total = part[0, pl.ds(rows, rows), pl.ds(which * wide, wide)]
        for d in range(2):
            k = last if which == d else last - 1
            rs[d][k].wait_recv()
            total = total + inbox[d, k].astype(jnp.float32)
        part[0, pl.ds(rows, rows), pl.ds(which * wide, wide)] = total
    total = part[0, pl.ds(rows, rows), :]
    scale = lax.rsqrt(jnp.mean(total * total, axis=1, keepdims=True) + EPS)
    mixed_ref[...] = (total * scale * post_ref[...]).astype(jnp.bfloat16)

    for copies in (*xs, *ys, *rs, cs):
        for copy in copies:
            copy.wait_send()


def solution(mesh):
    n_tp, n_fs = mesh.shape["tp"], mesh.shape["fs"]

    def per_device(prompt_tokens, up_weight, down_weight, pre_gain, post_gain):
        rows, width = prompt_tokens.shape
        shard, units = up_weight.shape
        x_steps, y_steps = len(ring_items(n_tp)), len(ring_items(n_fs // 2))
        vmem = pl.BlockSpec(memory_space=pltpu.VMEM)
        hbm = pl.BlockSpec(memory_space=pl.ANY)
        dma = pltpu.SemaphoreType.DMA
        return pl.pallas_call(
            functools.partial(kernel, n_tp, n_fs),
            out_shape=(
                jax.ShapeDtypeStruct((rows, width), jnp.bfloat16),
                jax.ShapeDtypeStruct((n_fs * shard, units), jnp.bfloat16),
                jax.ShapeDtypeStruct((n_fs * shard, units), jnp.bfloat16),
            ),
            in_specs=[hbm, hbm, hbm, vmem, vmem],
            out_specs=(vmem, vmem, vmem),
            scratch_shapes=[
                pltpu.VMEM((rows, width), jnp.bfloat16),
                pltpu.VMEM((shard, units), jnp.float32),
                pltpu.VMEM((shard, units), jnp.float32),
                pltpu.VMEM((n_tp // 2, 2 * rows, width), jnp.bfloat16),
                pltpu.VMEM((n_tp // 2, 2 * rows, units), jnp.bfloat16),
                pltpu.VMEM((n_tp // 2, 2 * rows, width), jnp.float32),
                pltpu.VMEM((2, x_steps, rows, width // 2), jnp.bfloat16),
                pltpu.VMEM((2, x_steps, rows, width // 2), jnp.bfloat16),
                dma((3,)),
                dma((2, x_steps)),
                dma((2, x_steps)),
                dma((2, y_steps)),
                dma((2, y_steps)),
                dma((2 + 2 * y_steps,)),
                dma((2 + 2 * y_steps,)),
                dma((2, x_steps)),
                dma((2, x_steps)),
            ],
            compiler_params=pltpu.CompilerParams(
                collective_id=0, has_side_effects=True, vmem_limit_bytes=56 * 2**20
            ),
        )(prompt_tokens, up_weight, down_weight, pre_gain[None, :], post_gain[None, :])

    placed = (P(("grp", "fs", "tp"), None), P("fs", "tp"), P("fs", "tp"), P("fs"), P())
    return jax.shard_map(
        per_device,
        mesh=mesh,
        in_specs=placed,
        out_specs=(P(("grp", "fs", "tp"), None), P("grp", "tp"), P("grp", "tp")),
        check_vma=False,
    )
```

```python
import functools

import jax
import jax.numpy as jnp
from jax import lax
from jax.experimental import pallas as pl
from jax.experimental.pallas import tpu as pltpu
from jax.sharding import PartitionSpec as P

MESH = pl.DeviceIdType.MESH
EPS = 1e-06
TILE = 256


def with_hops(chains):
    latest, count, slots = {}, {}, []
    for slot, chain in enumerate(chains):
        slots.append((chain, count.get(chain, 0), latest.get(chain, -1)))
        latest[chain], count[chain] = slot, count.get(chain, 0) + 1
    return slots


def far_first(n):
    far = n // 2
    chains = [c for r in range(far) for c in (0, 1, 2 + r % 2)]
    left = 2 * (far - 1) - far
    return with_hops(chains + [2 + k % 2 for k in range(left)])


def zero_and_two_first(n):
    far = n // 2
    chains = []
    for r in range(far):
        chains += [0] + [2] * (r < far - 1) + [1 if r % 2 == 0 else 3]
    ones, threes = far - chains.count(1), far - 1 - chains.count(3)
    for r in range(ones + threes):
        chains.append(1 if (ones + threes - r) % 2 else 3)
    return with_hops(chains)


def kernel(
    n_tp,
    n_fs,
    tok_hbm,
    up_hbm,
    down_hbm,
    pre_hbm,
    total_ref,
    wu,
    wd,
    tok_in,
    up_in,
    down_in,
    pre_in,
    tok,
    hid,
    part,
    outbox,
    inbox,
    in_sem,
    x_send,
    x_recv,
    y_send,
    y_recv,
    c_send,
    c_recv,
    r_send,
    r_recv,
):
    t = lax.axis_index("tp")
    f = lax.axis_index("fs")
    n_y = n_fs // 2
    y = f // 2
    x_peer = ({"tp": lax.rem(t + 1, n_tp)}, {"tp": lax.rem(t + n_tp - 1, n_tp)})
    y_peer = ({"fs": lax.rem(f + 2, n_fs)}, {"fs": lax.rem(f + n_fs - 2, n_fs)})
    core_peer = {"fs": f + 1 - 2 * lax.rem(f, 2)}
    rows, width = tok_in.shape
    shard = up_in.shape[0]
    strip = rows // 4
    wide = width // 4
    n_pairs = n_tp // 2

    barrier = pltpu.get_barrier_semaphore()
    for peer in (*x_peer, *y_peer, core_peer):
        pl.semaphore_signal(barrier, inc=1, device_id=peer, device_id_type=MESH)
    loads = [
        pltpu.make_async_copy(src, dst, in_sem.at[k])
        for k, (src, dst) in enumerate(((tok_hbm, tok_in), (pre_hbm, pre_in), (up_hbm, up_in), (down_hbm, down_in)))
    ]
    for load in loads:
        load.start()

    def shard_rows(index):
        return pl.ds(pl.multiple_of(index * shard, shard), shard)

    x_slots, y_slots = far_first(n_tp), zero_and_two_first(n_y)

    def tok_strip(direction, chain, distance):
        if distance == 0:
            pair, row = 0, rows
        elif distance == n_pairs:
            pair, row = 0, 0
        else:
            pair, row = distance, (rows if direction == 0 else 0)
        which = chain if direction == 0 else (chain + 2) % 4
        return tok.at[pair, pl.ds(row + which * strip, strip), :]

    def weight_piece(direction, chain, distance):
        step = 2 * distance
        owner = lax.rem(f + n_fs - step, n_fs) if direction == 0 else lax.rem(f + step, n_fs)
        part_of = chain // 2 if direction == 0 else 1 - chain // 2
        piece = pl.ds(pl.multiple_of(owner * shard + part_of * (shard // 2), shard // 2), shard // 2)
        return (wu, wd)[chain % 2].at[piece, :]

    def x_copy(direction, slot):
        chain, hop, _ = x_slots[slot]
        return pltpu.make_async_remote_copy(
            src_ref=tok_strip(direction, chain, hop),
            dst_ref=tok_strip(direction, chain, hop + 1),
            send_sem=x_send.at[direction, slot],
            recv_sem=x_recv.at[direction, slot],
            device_id=x_peer[direction],
            device_id_type=MESH,
        )

    def y_copy(direction, slot):
        chain, hop, _ = y_slots[slot]
        piece = weight_piece(direction, chain, hop)
        return pltpu.make_async_remote_copy(
            src_ref=piece,
            dst_ref=piece,
            send_sem=y_send.at[direction, slot],
            recv_sem=y_recv.at[direction, slot],
            device_id=y_peer[direction],
            device_id_type=MESH,
        )

    def core_copy(slot, piece):
        return pltpu.make_async_remote_copy(
            src_ref=piece,
            dst_ref=piece,
            send_sem=c_send.at[slot],
            recv_sem=c_recv.at[slot],
            device_id=core_peer,
            device_id_type=MESH,
        )

    def r_copy(direction, slot):
        return pltpu.make_async_remote_copy(
            src_ref=outbox.at[direction, slot],
            dst_ref=inbox.at[direction, slot],
            send_sem=r_send.at[direction, slot],
            recv_sem=r_recv.at[direction, slot],
            device_id=x_peer[direction],
            device_id_type=MESH,
        )

    xs = [[x_copy(d, k) for k in range(len(x_slots))] for d in range(2)]
    ys = [[y_copy(d, k) for k in range(len(y_slots))] for d in range(2)]
    rs = [[r_copy(d, k) for k in range(len(x_slots))] for d in range(2)]
    own = [core_copy(which, (wu, wd)[which].at[shard_rows(f), :]) for which in range(2)]
    across = [
        [
            core_copy(2 + d * len(y_slots) + k, weight_piece(d, chain, hop + 1))
            for k, (chain, hop, _) in enumerate(y_slots)
        ]
        for d in range(2)
    ]

    loads[0].wait()
    values = tok_in[...].astype(jnp.float32)
    scale = lax.rsqrt(jnp.mean(values * values, axis=1, keepdims=True) + EPS)
    tok[0, rows:, :] = (values * scale).astype(jnp.bfloat16)
    loads[1].wait()
    loads[2].wait()
    gain = jnp.broadcast_to(pre_in[...], (shard, shard)).T
    for c in range(up_in.shape[1] // shard):
        cols = pl.ds(c * shard, shard)
        wu[shard_rows(f), cols] = (up_in[:, cols] * gain).astype(jnp.bfloat16)

    pl.semaphore_wait(barrier, 5)

    started = {"x": 0, "y": 0}

    def go_on(name, copies, slots, received, limit):
        while started[name] < min(limit, len(slots)) and slots[started[name]][2] <= received:
            for d in range(2):
                copies[d][started[name]].start()
            started[name] += 1

    go_on("x", xs, x_slots, -1, 3)
    go_on("y", ys, y_slots, -1, 2)
    own[0].start()
    loads[3].wait()
    wd[shard_rows(f), :] = down_in[...].astype(jnp.bfloat16)
    go_on("y", ys, y_slots, -1, 3)
    own[1].start()

    settled = [-1]

    def settle(tick):
        if settled[0] == -1:
            own[0].wait_recv()
            own[1].wait_recv()
        for k in range(max(settled[0], 0), tick + 1):
            for d in range(2):
                across[d][k].wait_recv()
        settled[0] = max(settled[0], tick + 1)

    def tick(k):
        if k < len(y_slots):
            for d in range(2):
                ys[d][k].wait_recv()
            go_on("y", ys, y_slots, k, k + 4)
            for d in range(2):
                across[d][k].start()
        if k < len(x_slots):
            for d in range(2):
                xs[d][k].wait_recv()
            go_on("x", xs, x_slots, k, k + 4)

    def hidden(pair):
        def one(n, carry):
            cols = pl.ds(pl.multiple_of(n * TILE, TILE), TILE)
            lifted = jnp.dot(tok[pair], wu[:, cols], preferred_element_type=jnp.float32)
            lifted = jnp.maximum(lifted, 0.0)
            hid[pair, :, cols] = (lifted * lifted).astype(jnp.bfloat16)
            return carry

        lax.fori_loop(0, hid.shape[2] // TILE, one, 0)

    near = n_y // 4
    block = 2 * shard

    def features(quarter, n):
        away = n + (near if quarter >= 2 else 0)
        source = lax.rem(y + away, n_y) if quarter % 2 == 0 else lax.rem(y + n_y - 1 - away, n_y)
        return pl.ds(pl.multiple_of(source * block, block), block)

    def partial(pair, quarter):
        def one(n, carry):
            cols = pl.ds(pl.multiple_of(quarter * wide + n * block, block), block)
            part[pair, :, cols] = lax.dot_general(
                hid[pair],
                wd[features(quarter, n), :],
                (((1,), (1,)), ((), ())),
                preferred_element_type=jnp.float32,
            )
            return carry

        lax.fori_loop(0, near, one, 0)

    def quarter_of(direction, chain):
        return ((0, 2, 1, 3), (1, 3, 0, 2))[direction][chain]

    def ahead(slot):
        chain, hop, _ = x_slots[slot]
        return (n_pairs if chain < 2 else n_pairs - 1) - hop

    def pass_on(slot, directions=(0, 1)):
        chain, hop, before = x_slots[slot]
        steps = ahead(slot)
        for d in directions:
            pair, row = (0, 0) if steps == n_pairs else (steps, 0 if d == 0 else rows)
            mine = part[pair, pl.ds(row, rows), pl.ds(quarter_of(d, chain) * wide, wide)]
            if hop > 0:
                rs[d][before].wait_recv()
                mine = mine + inbox[d, before].astype(jnp.float32)
            outbox[d, slot] = mine.astype(jnp.bfloat16)
        for d in directions:
            rs[d][slot].start()

    last_y = {c: max(k for k, s in enumerate(y_slots) if s[0] == c) for c in range(4)}
    near_y = max(k for k, (c, hop, _) in enumerate(y_slots) if c % 2 == 1 and hop + 1 <= near)
    last_x = max(k for k, s in enumerate(x_slots) if s[0] < 2)
    ready = max(last_x, last_y[0], last_y[2], near_y)
    ticks = max(len(x_slots), len(y_slots))
    begin = min(ready + 1, ticks - 1)
    for k in range(begin + 1):
        tick(k)
    settle(ready)
    hidden(0)
    partial(0, 0)
    partial(0, 1)
    pass_on(0)
    for k in range(begin + 1, ticks):
        tick(k)
    settle(ticks - 2)
    partial(0, 2)
    pass_on(1, (0,))
    settle(ticks - 1)
    partial(0, 3)
    pass_on(1, (1,))

    slots = list(range(2, len(x_slots)))
    for pair in range(n_pairs - 1, 0, -1):
        hidden(pair)
        for quarters in ((0, 1), (2, 3)):
            for quarter in quarters:
                partial(pair, quarter)
            while slots:
                chain = x_slots[slots[0]][0]
                if ahead(slots[0]) < pair:
                    break
                if ahead(slots[0]) == pair and not {quarter_of(d, chain) for d in range(2)} <= set(range(quarters[-1] + 1)):
                    break
                pass_on(slots.pop(0))

    for quarter in (0, 1, 2, 3):
        total = part[0, pl.ds(rows, rows), pl.ds(quarter * wide, wide)]
        for d in range(2):
            slot = max(k for k, s in enumerate(x_slots) if quarter_of(d, s[0]) == quarter)
            rs[d][slot].wait_recv()
            total = total + inbox[d, slot].astype(jnp.float32)
        for n in range(near):
            total_ref[:, features(quarter, n)] = total[:, n * block : (n + 1) * block]

    for copies in (*xs, *ys, *rs, own, *across):
        for copy in copies:
            copy.wait_send()


def finish(total_ref, wu, wd, post_hbm, mixed_hbm, up_hbm, down_hbm, mixed, post, sem):
    load = pltpu.make_async_copy(post_hbm, post, sem.at[3])
    load.start()
    copies = [
        pltpu.make_async_copy(src, dst, sem.at[k])
        for k, (src, dst) in enumerate(((wu, up_hbm), (wd, down_hbm), (mixed, mixed_hbm)))
    ]
    copies[0].start()
    copies[1].start()
    total = total_ref[...]
    scale = lax.rsqrt(jnp.mean(total * total, axis=1, keepdims=True) + EPS)
    load.wait()
    mixed[...] = (total * scale * post[...]).astype(jnp.bfloat16)
    copies[2].start()
    for copy in copies:
        copy.wait()


def solution(mesh):
    n_tp, n_fs = mesh.shape["tp"], mesh.shape["fs"]

    def per_device(*arrays):
        prompt_tokens, up_weight, down_weight, pre_gain, post_gain = (
            pltpu.with_memory_space_constraint(a[None, :] if a.ndim == 1 else a, pltpu.HBM) for a in arrays
        )
        rows, width = prompt_tokens.shape
        shard, units = up_weight.shape
        x_steps, y_steps = len(far_first(n_tp)), len(zero_and_two_first(n_fs // 2))
        vmem = pl.BlockSpec(memory_space=pltpu.VMEM)
        hbm = pl.BlockSpec(memory_space=pltpu.HBM)
        dma = pltpu.SemaphoreType.DMA
        total, sampler_up, sampler_down = pl.pallas_call(
            functools.partial(kernel, n_tp, n_fs),
            out_shape=(
                pltpu.VMEM((rows, width), jnp.float32),
                pltpu.VMEM((n_fs * shard, units), jnp.bfloat16),
                pltpu.VMEM((n_fs * shard, units), jnp.bfloat16),
            ),
            in_specs=[hbm, hbm, hbm, hbm],
            out_specs=(vmem, vmem, vmem),
            scratch_shapes=[
                pltpu.VMEM((rows, width), jnp.bfloat16),
                pltpu.VMEM((shard, units), jnp.float32),
                pltpu.VMEM((shard, units), jnp.float32),
                pltpu.VMEM((1, shard), jnp.float32),
                pltpu.VMEM((n_tp // 2, 2 * rows, width), jnp.bfloat16),
                pltpu.VMEM((n_tp // 2, 2 * rows, units), jnp.bfloat16),
                pltpu.VMEM((n_tp // 2, 2 * rows, width), jnp.float32),
                pltpu.VMEM((2, x_steps, rows, width // 4), jnp.bfloat16),
                pltpu.VMEM((2, x_steps, rows, width // 4), jnp.bfloat16),
                dma((4,)),
                dma((2, x_steps)),
                dma((2, x_steps)),
                dma((2, y_steps)),
                dma((2, y_steps)),
                dma((2 + 2 * y_steps,)),
                dma((2 + 2 * y_steps,)),
                dma((2, x_steps)),
                dma((2, x_steps)),
            ],
            compiler_params=pltpu.CompilerParams(
                collective_id=0, has_side_effects=True, vmem_limit_bytes=42 * 2**20
            ),
        )(prompt_tokens, up_weight, down_weight, pre_gain)
        return pl.pallas_call(
            finish,
            out_shape=(
                jax.ShapeDtypeStruct((rows, width), jnp.bfloat16),
                jax.ShapeDtypeStruct((n_fs * shard, units), jnp.bfloat16),
                jax.ShapeDtypeStruct((n_fs * shard, units), jnp.bfloat16),
            ),
            in_specs=[vmem, vmem, vmem, hbm],
            out_specs=(hbm, hbm, hbm),
            scratch_shapes=[
                pltpu.VMEM((rows, width), jnp.bfloat16),
                pltpu.VMEM((1, width), jnp.float32),
                dma((4,)),
            ],
            compiler_params=pltpu.CompilerParams(vmem_limit_bytes=16 * 2**20),
        )(total, sampler_up, sampler_down, post_gain)

    placed = (P(("grp", "fs", "tp"), None), P("fs", "tp"), P("fs", "tp"), P("fs"), P())
    return jax.shard_map(
        per_device,
        mesh=mesh,
        in_specs=placed,
        out_specs=(P(("grp", "fs", "tp"), None), P("grp", "tp"), P("grp", "tp")),
        check_vma=False,
    )
```

```python
import functools

import jax
import jax.numpy as jnp
from jax import lax
from jax.experimental import pallas as pl
from jax.experimental.pallas import tpu as pltpu
from jax.sharding import PartitionSpec as P

MESH = pl.DeviceIdType.MESH
EPS = 1e-06
TILE = 256


def with_hops(chains):
    latest, count, slots = {}, {}, []
    for slot, chain in enumerate(chains):
        slots.append((chain, count.get(chain, 0), latest.get(chain, -1)))
        latest[chain], count[chain] = slot, count.get(chain, 0) + 1
    return slots


def far_first(n):
    far = n // 2
    chains = [c for r in range(far) for c in (0, 1, 2 + r % 2)]
    left = 2 * (far - 1) - far
    return with_hops(chains + [2 + k % 2 for k in range(left)])


def zero_and_two_first(n):
    far = n // 2
    chains = []
    for r in range(far):
        chains += [0] + [2] * (r < far - 1) + [1 if r % 2 == 0 else 3]
    ones, threes = far - chains.count(1), far - 1 - chains.count(3)
    for r in range(ones + threes):
        chains.append(1 if (ones + threes - r) % 2 else 3)
    return with_hops(chains)


def near_first(n):
    far = n // 2
    chains, left = [0, 2, 0], {0: far - 2, 1: far, 2: far - 2, 3: far - 1}
    turn = (1, 2, 0, 3)
    while any(left.values()):
        for c in turn:
            if left[c] > 0:
                chains.append(c)
                left[c] -= 1
    return with_hops(chains)


def kernel(
    n_tp,
    n_fs,
    tok_hbm,
    up_hbm,
    down_hbm,
    pre_hbm,
    total_ref,
    wu,
    wd,
    tok_in,
    up_in,
    down_in,
    pre_in,
    tok,
    hid,
    part,
    outbox,
    inbox,
    in_sem,
    x_send,
    x_recv,
    y_send,
    y_recv,
    c_send,
    c_recv,
    r_send,
    r_recv,
    here,
):
    t = lax.axis_index("tp")
    f = lax.axis_index("fs")
    n_y = n_fs // 2
    y = f // 2
    x_peer = ({"tp": lax.rem(t + 1, n_tp)}, {"tp": lax.rem(t + n_tp - 1, n_tp)})
    y_peer = ({"fs": lax.rem(f + 2, n_fs)}, {"fs": lax.rem(f + n_fs - 2, n_fs)})
    core_peer = {"fs": f + 1 - 2 * lax.rem(f, 2)}
    rows, width = tok_in.shape
    shard = up_in.shape[0]
    strip = rows // 4
    wide = width // 4
    n_pairs = n_tp // 2

    core = lax.rem(f, 2)
    first_row, last_row = y == 0, y == n_y - 1
    barrier = pltpu.get_barrier_semaphore()

    def tell(semaphore, peer):
        pl.semaphore_signal(semaphore, inc=1, device_id=peer, device_id_type=MESH)

    for peer in x_peer:
        tell(barrier, peer)
    pl.when(jnp.logical_not(last_row))(lambda: tell(barrier, y_peer[0]))
    pl.when(first_row)(lambda: tell(barrier, y_peer[1]))
    pl.when(core == 1)(lambda: tell(barrier, core_peer))
    loads = [
        pltpu.make_async_copy(src, dst, in_sem.at[k])
        for k, (src, dst) in enumerate(((tok_hbm, tok_in), (pre_hbm, pre_in), (up_hbm, up_in), (down_hbm, down_in)))
    ]
    for load in loads:
        load.start()

    def shard_rows(index):
        return pl.ds(pl.multiple_of(index * shard, shard), shard)

    x_slots, y_slots, r_slots = far_first(n_tp), zero_and_two_first(n_y), near_first(n_tp)

    def tok_strip(direction, chain, distance):
        if distance == 0:
            pair, row = 0, rows
        elif distance == n_pairs:
            pair, row = 0, 0
        else:
            pair, row = distance, (rows if direction == 0 else 0)
        which = chain if direction == 0 else (chain + 2) % 4
        return tok.at[pair, pl.ds(row + which * strip, strip), :]

    def weight_piece(direction, chain, distance):
        step = 2 * distance
        owner = lax.rem(f + n_fs - step, n_fs) if direction == 0 else lax.rem(f + step, n_fs)
        part_of = chain // 2 if direction == 0 else 1 - chain // 2
        piece = pl.ds(pl.multiple_of(owner * shard + part_of * (shard // 2), shard // 2), shard // 2)
        return (wu, wd)[chain % 2].at[piece, :]

    def x_copy(direction, slot):
        chain, hop, _ = x_slots[slot]
        return pltpu.make_async_remote_copy(
            src_ref=tok_strip(direction, chain, hop),
            dst_ref=tok_strip(direction, chain, hop + 1),
            send_sem=x_send.at[direction, slot],
            recv_sem=x_recv.at[direction, slot],
            device_id=x_peer[direction],
            device_id_type=MESH,
        )

    def y_copy(direction, slot):
        chain, hop, _ = y_slots[slot]
        piece = weight_piece(direction, chain, hop)
        return pltpu.make_async_remote_copy(
            src_ref=piece,
            dst_ref=piece,
            send_sem=y_send.at[direction, slot],
            recv_sem=y_recv.at[direction, slot],
            device_id=y_peer[direction],
            device_id_type=MESH,
        )

    def core_copy(slot, piece):
        return pltpu.make_async_remote_copy(
            src_ref=piece,
            dst_ref=piece,
            send_sem=c_send.at[slot],
            recv_sem=c_recv.at[slot],
            device_id=core_peer,
            device_id_type=MESH,
        )

    def r_copy(direction, slot):
        return pltpu.make_async_remote_copy(
            src_ref=outbox.at[direction, slot],
            dst_ref=inbox.at[direction, slot],
            send_sem=r_send.at[direction, slot],
            recv_sem=r_recv.at[direction, slot],
            device_id=x_peer[direction],
            device_id_type=MESH,
        )

    xs = [[x_copy(d, k) for k in range(len(x_slots))] for d in range(2)]
    ys = [[y_copy(d, k) for k in range(len(y_slots))] for d in range(2)]
    rs = [[r_copy(d, k) for k in range(len(x_slots))] for d in range(2)]
    own = [core_copy(which, (wu, wd)[which].at[shard_rows(f), :]) for which in range(2)]
    across = [
        [
            core_copy(2 + d * len(y_slots) + k, weight_piece(d, chain, hop + 1))
            for k, (chain, hop, _) in enumerate(y_slots)
        ]
        for d in range(2)
    ]

    loads[0].wait()
    values = tok_in[...].astype(jnp.float32)
    scale = lax.rsqrt(jnp.mean(values * values, axis=1, keepdims=True) + EPS)
    tok[0, rows:, :] = (values * scale).astype(jnp.bfloat16)
    awaited = 2 + (y > 0).astype(jnp.int32) + last_row.astype(jnp.int32) + (1 - core)
    pl.semaphore_wait(barrier, awaited)
    pl.when(y > 0)(lambda: tell(here.at[0], y_peer[1]))
    pl.when(last_row)(lambda: tell(here.at[1], y_peer[0]))
    pl.when(core == 0)(lambda: tell(here.at[2], core_peer))

    started = {"x": 0, "y": 0}

    def go_on(name, copies, slots, received, limit):
        while started[name] < min(limit, len(slots)) and slots[started[name]][2] <= received:
            for d in range(2):
                copies[d][started[name]].start()
            started[name] += 1

    go_on("x", xs, x_slots, -1, 3)

    loads[1].wait()
    loads[2].wait()
    gain = jnp.broadcast_to(pre_in[...], (shard, shard)).T
    for c in range(up_in.shape[1] // shard):
        cols = pl.ds(c * shard, shard)
        wu[shard_rows(f), cols] = (up_in[:, cols] * gain).astype(jnp.bfloat16)
    loads[3].wait()
    wd[shard_rows(f), :] = down_in[...].astype(jnp.bfloat16)

    settled = [-1]

    def settle(tick):
        if settled[0] == -1:
            own[0].wait_recv()
            own[1].wait_recv()
        for k in range(max(settled[0], 0), tick + 1):
            for d in range(2):
                across[d][k].wait_recv()
        settled[0] = max(settled[0], tick + 1)

    def x_tick(k):
        if k < len(x_slots):
            for d in range(2):
                xs[d][k].wait_recv()
            go_on("x", xs, x_slots, k, k + 4)

    def y_begin():
        pl.when(jnp.logical_not(last_row))(lambda: pl.semaphore_wait(here.at[0], 1))
        pl.when(first_row)(lambda: pl.semaphore_wait(here.at[1], 1))
        go_on("y", ys, y_slots, -1, 3)

    meet = len(y_slots) // 2

    def y_tick(k):
        for d in range(2):
            ys[d][k].wait_recv()
        go_on("y", ys, y_slots, k, k + 4)
        if k == meet:
            pl.when(core == 1)(lambda: pl.semaphore_wait(here.at[2], 1))
            for copy in own:
                copy.start()
        if k >= meet:
            for j in range(0 if k == meet else k, k + 1):
                for d in range(2):
                    across[d][j].start()

    def hidden(pair):
        def one(n, carry):
            cols = pl.ds(pl.multiple_of(n * TILE, TILE), TILE)
            lifted = jnp.dot(tok[pair], wu[:, cols], preferred_element_type=jnp.float32)
            lifted = jnp.maximum(lifted, 0.0)
            hid[pair, :, cols] = (lifted * lifted).astype(jnp.bfloat16)
            return carry

        lax.fori_loop(0, hid.shape[2] // TILE, one, 0)

    near = n_y // 4
    block = 2 * shard

    def features(quarter, n):
        away = n + (near if quarter >= 2 else 0)
        source = lax.rem(y + away, n_y) if quarter % 2 == 0 else lax.rem(y + n_y - 1 - away, n_y)
        return pl.ds(pl.multiple_of(source * block, block), block)

    def partial(pair, quarter):
        def one(n, carry):
            cols = pl.ds(pl.multiple_of(quarter * wide + n * block, block), block)
            part[pair, :, cols] = lax.dot_general(
                hid[pair],
                wd[features(quarter, n), :],
                (((1,), (1,)), ((), ())),
                preferred_element_type=jnp.float32,
            )
            return carry

        lax.fori_loop(0, near, one, 0)

    def quarter_of(direction, chain):
        return ((0, 2, 1, 3), (1, 3, 0, 2))[direction][chain]

    def ahead(slot):
        chain, hop, _ = r_slots[slot]
        return (n_pairs if chain < 2 else n_pairs - 1) - hop

    def pass_on(slot, directions=(0, 1)):
        chain, hop, before = r_slots[slot]
        steps = ahead(slot)
        for d in directions:
            pair, row = (0, 0) if steps == n_pairs else (steps, 0 if d == 0 else rows)
            mine = part[pair, pl.ds(row, rows), pl.ds(quarter_of(d, chain) * wide, wide)]
            if hop > 0:
                rs[d][before].wait_recv()
                mine = mine + inbox[d, before].astype(jnp.float32)
            outbox[d, slot] = mine.astype(jnp.bfloat16)
        for d in directions:
            rs[d][slot].start()

    ups = max(k for k, s in enumerate(y_slots) if s[0] % 2 == 0)
    nears = max(k for k, (c, hop, _) in enumerate(y_slots) if c % 2 == 1 and hop + 1 <= near)
    nears = max(nears, ups)
    far_x = max(k for k, s in enumerate(x_slots) if s[0] < 2)
    last, last_w = len(x_slots) - 1, len(y_slots) - 1

    def first_half(lag):
        started.update(x=3, y=0)
        settled[0] = -1
        done = {"x": 0, "y": 0}
        y_begin()

        def gather(x_until, y_until):
            while done["x"] <= x_until or done["y"] <= y_until:
                if done["x"] <= last and done["x"] <= done["y"] + lag:
                    x_tick(done["x"])
                    done["x"] += 1
                else:
                    y_tick(done["y"])
                    done["y"] += 1

        gather(min(far_x + 1, last), min(ups + 1, last_w))
        settle(ups)
        hidden(0)
        gather(min(far_x + 2, last), min(nears + 1, last_w))
        settle(nears)
        partial(0, 0)
        partial(0, 1)
        pass_on(0)
        gather(last, min(nears + 1, last_w))
        hidden(n_pairs - 1)
        partial(n_pairs - 1, 0)
        partial(n_pairs - 1, 1)
        pass_on(1)
        gather(last, min(nears + 2, last_w))
        pass_on(2)
        gather(last, last_w)
        settle(last_w)

    first_half(1)
    n_slots = len(x_slots)
    partial(0, 2)
    partial(0, 3)

    have = {(0, q) for q in range(4)} | {(n_pairs - 1, q) for q in range(2)}
    lifted_pairs = {0, n_pairs - 1}
    for slot in range(3, n_slots):
        pair = ahead(slot) % n_pairs
        if pair not in lifted_pairs:
            hidden(pair)
            lifted_pairs.add(pair)
        for d in range(2):
            quarter = quarter_of(d, r_slots[slot][0])
            if (pair, quarter) not in have:
                partial(pair, quarter)
                have.add((pair, quarter))
        pass_on(slot)

    for quarter in (0, 1, 2, 3):
        total = part[0, pl.ds(rows, rows), pl.ds(quarter * wide, wide)]
        for d in range(2):
            slot = max(k for k, s in enumerate(r_slots) if quarter_of(d, s[0]) == quarter)
            rs[d][slot].wait_recv()
            total = total + inbox[d, slot].astype(jnp.float32)
        for n in range(near):
            total_ref[:, features(quarter, n)] = total[:, n * block : (n + 1) * block]

    for copies in (*xs, *ys, *rs, own, *across):
        for copy in copies:
            copy.wait_send()


def finish(total_ref, wu, wd, post_hbm, mixed_hbm, up_hbm, down_hbm, mixed, post, sem):
    load = pltpu.make_async_copy(post_hbm, post, sem.at[3])
    load.start()
    copies = [
        pltpu.make_async_copy(src, dst, sem.at[k])
        for k, (src, dst) in enumerate(((wu, up_hbm), (wd, down_hbm), (mixed, mixed_hbm)))
    ]
    copies[0].start()
    copies[1].start()
    total = total_ref[...]
    scale = lax.rsqrt(jnp.mean(total * total, axis=1, keepdims=True) + EPS)
    load.wait()
    mixed[...] = (total * scale * post[...]).astype(jnp.bfloat16)
    copies[2].start()
    for copy in copies:
        copy.wait()


def solution(mesh):
    n_tp, n_fs = mesh.shape["tp"], mesh.shape["fs"]

    def per_device(*arrays):
        prompt_tokens, up_weight, down_weight, pre_gain, post_gain = (
            pltpu.with_memory_space_constraint(a[None, :] if a.ndim == 1 else a, pltpu.HBM) for a in arrays
        )
        rows, width = prompt_tokens.shape
        shard, units = up_weight.shape
        x_steps, y_steps = len(far_first(n_tp)), len(zero_and_two_first(n_fs // 2))
        vmem = pl.BlockSpec(memory_space=pltpu.VMEM)
        hbm = pl.BlockSpec(memory_space=pltpu.HBM)
        dma = pltpu.SemaphoreType.DMA
        total, sampler_up, sampler_down = pl.pallas_call(
            functools.partial(kernel, n_tp, n_fs),
            out_shape=(
                pltpu.VMEM((rows, width), jnp.float32),
                pltpu.VMEM((n_fs * shard, units), jnp.bfloat16),
                pltpu.VMEM((n_fs * shard, units), jnp.bfloat16),
            ),
            in_specs=[hbm, hbm, hbm, hbm],
            out_specs=(vmem, vmem, vmem),
            scratch_shapes=[
                pltpu.VMEM((rows, width), jnp.bfloat16),
                pltpu.VMEM((shard, units), jnp.float32),
                pltpu.VMEM((shard, units), jnp.float32),
                pltpu.VMEM((1, shard), jnp.float32),
                pltpu.VMEM((n_tp // 2, 2 * rows, width), jnp.bfloat16),
                pltpu.VMEM((n_tp // 2, 2 * rows, units), jnp.bfloat16),
                pltpu.VMEM((n_tp // 2, 2 * rows, width), jnp.float32),
                pltpu.VMEM((2, x_steps, rows, width // 4), jnp.bfloat16),
                pltpu.VMEM((2, x_steps, rows, width // 4), jnp.bfloat16),
                dma((4,)),
                dma((2, x_steps)),
                dma((2, x_steps)),
                dma((2, y_steps)),
                dma((2, y_steps)),
                dma((2 + 2 * y_steps,)),
                dma((2 + 2 * y_steps,)),
                dma((2, x_steps)),
                dma((2, x_steps)),
                pltpu.SemaphoreType.REGULAR((3,)),
            ],
            compiler_params=pltpu.CompilerParams(
                collective_id=0, has_side_effects=True, vmem_limit_bytes=42 * 2**20
            ),
        )(prompt_tokens, up_weight, down_weight, pre_gain)
        return pl.pallas_call(
            finish,
            out_shape=(
                jax.ShapeDtypeStruct((rows, width), jnp.bfloat16),
                jax.ShapeDtypeStruct((n_fs * shard, units), jnp.bfloat16),
                jax.ShapeDtypeStruct((n_fs * shard, units), jnp.bfloat16),
            ),
            in_specs=[vmem, vmem, vmem, hbm],
            out_specs=(hbm, hbm, hbm),
            scratch_shapes=[
                pltpu.VMEM((rows, width), jnp.bfloat16),
                pltpu.VMEM((1, width), jnp.float32),
                dma((4,)),
            ],
            compiler_params=pltpu.CompilerParams(vmem_limit_bytes=16 * 2**20),
        )(total, sampler_up, sampler_down, post_gain)

    placed = (P(("grp", "fs", "tp"), None), P("fs", "tp"), P("fs", "tp"), P("fs"), P())
    return jax.shard_map(
        per_device,
        mesh=mesh,
        in_specs=placed,
        out_specs=(P(("grp", "fs", "tp"), None), P("grp", "tp"), P("grp", "tp")),
        check_vma=False,
    )
```

```python
import functools

import jax
import jax.numpy as jnp
from jax import lax
from jax.experimental import pallas as pl
from jax.experimental.pallas import tpu as pltpu
from jax.sharding import PartitionSpec as P

MESH = pl.DeviceIdType.MESH
EPS = 1e-06
TILE = 256


def with_hops(chains):
    latest, count, slots = {}, {}, []
    for slot, chain in enumerate(chains):
        slots.append((chain, count.get(chain, 0), latest.get(chain, -1)))
        latest[chain], count[chain] = slot, count.get(chain, 0) + 1
    return slots


def far_first(n):
    far = n // 2
    chains = [c for r in range(far) for c in (0, 1, 2 + r % 2)]
    left = 2 * (far - 1) - far
    return with_hops(chains + [2 + k % 2 for k in range(left)])


def zero_and_two_first(n):
    far = n // 2
    chains = []
    for r in range(far):
        chains += [0] + [2] * (r < far - 1) + [1 if r % 2 == 0 else 3]
    ones, threes = far - chains.count(1), far - 1 - chains.count(3)
    for r in range(ones + threes):
        chains.append(1 if (ones + threes - r) % 2 else 3)
    return with_hops(chains)


def near_first(n):
    far = n // 2
    chains, left = [0, 2, 0], {0: far - 2, 1: far, 2: far - 2, 3: far - 1}
    turn = (1, 2, 0, 3)
    while any(left.values()):
        for c in turn:
            if left[c] > 0:
                chains.append(c)
                left[c] -= 1
    return with_hops(chains)


def kernel(
    n_tp,
    n_fs,
    tok_hbm,
    up_hbm,
    down_hbm,
    pre_hbm,
    total_ref,
    wu,
    wd,
    tok_in,
    up_in,
    down_in,
    pre_in,
    tok,
    hid,
    part,
    outbox,
    inbox,
    in_sem,
    x_send,
    x_recv,
    y_send,
    y_recv,
    c_send,
    c_recv,
    r_send,
    r_recv,
    here,
):
    t = lax.axis_index("tp")
    f = lax.axis_index("fs")
    n_y = n_fs // 2
    y = f // 2
    x_peer = ({"tp": lax.rem(t + 1, n_tp)}, {"tp": lax.rem(t + n_tp - 1, n_tp)})
    y_peer = ({"fs": lax.rem(f + 2, n_fs)}, {"fs": lax.rem(f + n_fs - 2, n_fs)})
    core_peer = {"fs": f + 1 - 2 * lax.rem(f, 2)}
    rows, width = tok_in.shape
    shard = up_in.shape[0]
    strip = rows // 4
    wide = width // 4
    n_pairs = n_tp // 2

    core = lax.rem(f, 2)
    first_row, last_row = y == 0, y == n_y - 1
    barrier = pltpu.get_barrier_semaphore()

    def tell(semaphore, peer):
        pl.semaphore_signal(semaphore, inc=1, device_id=peer, device_id_type=MESH)

    for peer in x_peer:
        tell(barrier, peer)
    pl.when(jnp.logical_not(last_row))(lambda: tell(barrier, y_peer[0]))
    pl.when(first_row)(lambda: tell(barrier, y_peer[1]))
    pl.when(core == 1)(lambda: tell(barrier, core_peer))
    loads = [
        pltpu.make_async_copy(src, dst, in_sem.at[k])
        for k, (src, dst) in enumerate(((tok_hbm, tok_in), (pre_hbm, pre_in), (up_hbm, up_in), (down_hbm, down_in)))
    ]
    for load in loads:
        load.start()

    def shard_rows(index):
        return pl.ds(pl.multiple_of(index * shard, shard), shard)

    x_slots, y_slots, r_slots = far_first(n_tp), zero_and_two_first(n_y), near_first(n_tp)

    def tok_strip(direction, chain, distance):
        if distance == 0:
            pair, row = 0, rows
        elif distance == n_pairs:
            pair, row = 0, 0
        else:
            pair, row = distance, (rows if direction == 0 else 0)
        which = chain if direction == 0 else (chain + 2) % 4
        return tok.at[pair, pl.ds(row + which * strip, strip), :]

    def weight_piece(direction, chain, distance):
        step = 2 * distance
        owner = lax.rem(f + n_fs - step, n_fs) if direction == 0 else lax.rem(f + step, n_fs)
        part_of = chain // 2 if direction == 0 else 1 - chain // 2
        piece = pl.ds(pl.multiple_of(owner * shard + part_of * (shard // 2), shard // 2), shard // 2)
        return (wu, wd)[chain % 2].at[piece, :]

    def x_copy(direction, slot):
        chain, hop, _ = x_slots[slot]
        return pltpu.make_async_remote_copy(
            src_ref=tok_strip(direction, chain, hop),
            dst_ref=tok_strip(direction, chain, hop + 1),
            send_sem=x_send.at[direction, slot],
            recv_sem=x_recv.at[direction, slot],
            device_id=x_peer[direction],
            device_id_type=MESH,
        )

    def y_copy(direction, slot):
        chain, hop, _ = y_slots[slot]
        piece = weight_piece(direction, chain, hop)
        return pltpu.make_async_remote_copy(
            src_ref=piece,
            dst_ref=piece,
            send_sem=y_send.at[direction, slot],
            recv_sem=y_recv.at[direction, slot],
            device_id=y_peer[direction],
            device_id_type=MESH,
        )

    def core_copy(slot, piece):
        return pltpu.make_async_remote_copy(
            src_ref=piece,
            dst_ref=piece,
            send_sem=c_send.at[slot],
            recv_sem=c_recv.at[slot],
            device_id=core_peer,
            device_id_type=MESH,
        )

    def r_copy(direction, slot):
        return pltpu.make_async_remote_copy(
            src_ref=outbox.at[direction, slot],
            dst_ref=inbox.at[direction, slot],
            send_sem=r_send.at[direction, slot],
            recv_sem=r_recv.at[direction, slot],
            device_id=x_peer[direction],
            device_id_type=MESH,
        )

    xs = [[x_copy(d, k) for k in range(len(x_slots))] for d in range(2)]
    ys = [[y_copy(d, k) for k in range(len(y_slots))] for d in range(2)]
    rs = [[r_copy(d, k) for k in range(len(x_slots))] for d in range(2)]
    own = [core_copy(which, (wu, wd)[which].at[shard_rows(f), :]) for which in range(2)]
    across = [
        [
            core_copy(2 + d * len(y_slots) + k, weight_piece(d, chain, hop + 1))
            for k, (chain, hop, _) in enumerate(y_slots)
        ]
        for d in range(2)
    ]

    loads[0].wait()
    values = tok_in[...].astype(jnp.float32)
    scale = lax.rsqrt(jnp.mean(values * values, axis=1, keepdims=True) + EPS)
    tok[0, rows:, :] = (values * scale).astype(jnp.bfloat16)
    awaited = 2 + (y > 0).astype(jnp.int32) + last_row.astype(jnp.int32) + (1 - core)
    pl.semaphore_wait(barrier, awaited)
    pl.when(y > 0)(lambda: tell(here.at[0], y_peer[1]))
    pl.when(last_row)(lambda: tell(here.at[1], y_peer[0]))
    pl.when(core == 0)(lambda: tell(here.at[2], core_peer))

    started = {"x": 0, "y": 0}

    def go_on(name, copies, slots, received, limit):
        while started[name] < min(limit, len(slots)) and slots[started[name]][2] <= received:
            for d in range(2):
                copies[d][started[name]].start()
            started[name] += 1

    go_on("x", xs, x_slots, -1, 3)

    loads[1].wait()
    loads[2].wait()
    gain = jnp.broadcast_to(pre_in[...], (shard, shard)).T
    for c in range(up_in.shape[1] // shard):
        cols = pl.ds(c * shard, shard)
        wu[shard_rows(f), cols] = (up_in[:, cols] * gain).astype(jnp.bfloat16)
    loads[3].wait()
    wd[shard_rows(f), :] = down_in[...].astype(jnp.bfloat16)

    settled = [-1]

    def settle(tick):
        if settled[0] == -1:
            own[0].wait_recv()
            own[1].wait_recv()
        for k in range(max(settled[0], 0), tick + 1):
            for d in range(2):
                across[d][k].wait_recv()
        settled[0] = max(settled[0], tick + 1)

    def x_tick(k):
        if k < len(x_slots):
            for d in range(2):
                xs[d][k].wait_recv()
            go_on("x", xs, x_slots, k, k + 4)

    def y_begin():
        pl.when(jnp.logical_not(last_row))(lambda: pl.semaphore_wait(here.at[0], 1))
        pl.when(first_row)(lambda: pl.semaphore_wait(here.at[1], 1))
        go_on("y", ys, y_slots, -1, 3)

        @pl.when(core == 0)
        def _():
            for copy in own:
                copy.start()

    meet = len(y_slots) // 2

    def y_tick(k):
        for d in range(2):
            ys[d][k].wait_recv()
        go_on("y", ys, y_slots, k, k + 4)
        @pl.when(core == 0)
        def _():
            for d in range(2):
                across[d][k].start()

        if k >= meet:

            @pl.when(core == 1)
            def _():
                if k == meet:
                    pl.semaphore_wait(here.at[2], 1)
                    for copy in own:
                        copy.start()
                for j in range(0 if k == meet else k, k + 1):
                    for d in range(2):
                        across[d][j].start()

    def hidden(pair):
        def one(n, carry):
            cols = pl.ds(pl.multiple_of(n * TILE, TILE), TILE)
            lifted = jnp.dot(tok[pair], wu[:, cols], preferred_element_type=jnp.float32)
            lifted = jnp.maximum(lifted, 0.0)
            hid[pair, :, cols] = (lifted * lifted).astype(jnp.bfloat16)
            return carry

        lax.fori_loop(0, hid.shape[2] // TILE, one, 0)

    near = n_y // 4
    block = 2 * shard

    def features(quarter, n):
        away = n + (near if quarter >= 2 else 0)
        source = lax.rem(y + away, n_y) if quarter % 2 == 0 else lax.rem(y + n_y - 1 - away, n_y)
        return pl.ds(pl.multiple_of(source * block, block), block)

    def partial(pair, quarter):
        def one(n, carry):
            cols = pl.ds(pl.multiple_of(quarter * wide + n * block, block), block)
            part[pair, :, cols] = lax.dot_general(
                hid[pair],
                wd[features(quarter, n), :],
                (((1,), (1,)), ((), ())),
                preferred_element_type=jnp.float32,
            )
            return carry

        lax.fori_loop(0, near, one, 0)

    def quarter_of(direction, chain):
        return ((0, 2, 1, 3), (1, 3, 0, 2))[direction][chain]

    def ahead(slot):
        chain, hop, _ = r_slots[slot]
        return (n_pairs if chain < 2 else n_pairs - 1) - hop

    def pass_on(slot, directions=(0, 1)):
        chain, hop, before = r_slots[slot]
        steps = ahead(slot)
        for d in directions:
            pair, row = (0, 0) if steps == n_pairs else (steps, 0 if d == 0 else rows)
            mine = part[pair, pl.ds(row, rows), pl.ds(quarter_of(d, chain) * wide, wide)]
            if hop > 0:
                rs[d][before].wait_recv()
                mine = mine + inbox[d, before].astype(jnp.float32)
            outbox[d, slot] = mine.astype(jnp.bfloat16)
        for d in directions:
            rs[d][slot].start()

    ups = max(k for k, s in enumerate(y_slots) if s[0] % 2 == 0)
    nears = max(k for k, (c, hop, _) in enumerate(y_slots) if c % 2 == 1 and hop + 1 <= near)
    nears = max(nears, ups)
    far_x = max(k for k, s in enumerate(x_slots) if s[0] < 2)
    last, last_w = len(x_slots) - 1, len(y_slots) - 1

    def first_half(lag):
        started.update(x=3, y=0)
        settled[0] = -1
        done = {"x": 0, "y": 0}
        y_begin()

        def gather(x_until, y_until):
            while done["x"] <= x_until or done["y"] <= y_until:
                if done["x"] <= last and done["x"] <= done["y"] + lag:
                    x_tick(done["x"])
                    done["x"] += 1
                else:
                    y_tick(done["y"])
                    done["y"] += 1

        gather(min(far_x + 1, last), min(ups + 1, last_w))
        settle(ups)
        hidden(0)
        gather(min(far_x + 2, last), min(nears + 1, last_w))
        settle(nears)
        partial(0, 0)
        partial(0, 1)
        pass_on(0)
        gather(last, min(nears + 1, last_w))
        hidden(n_pairs - 1)
        partial(n_pairs - 1, 1)
        pass_on(1, (0,))
        partial(n_pairs - 1, 0)
        pass_on(1, (1,))
        gather(last, min(nears + 2, last_w))
        pass_on(2)
        gather(last, last_w)
        settle(last_w)

    first_half(1)
    n_slots = len(x_slots)
    partial(0, 2)
    partial(0, 3)

    have = {(0, q) for q in range(4)} | {(n_pairs - 1, q) for q in range(2)}
    lifted_pairs = {0, n_pairs - 1}
    for slot in range(3, n_slots):
        pair = ahead(slot) % n_pairs
        if pair not in lifted_pairs:
            hidden(pair)
            lifted_pairs.add(pair)
        for d in range(2):
            quarter = quarter_of(d, r_slots[slot][0])
            if (pair, quarter) not in have:
                partial(pair, quarter)
                have.add((pair, quarter))
        pass_on(slot)

    for quarter in (0, 1, 2, 3):
        total = part[0, pl.ds(rows, rows), pl.ds(quarter * wide, wide)]
        for d in range(2):
            slot = max(k for k, s in enumerate(r_slots) if quarter_of(d, s[0]) == quarter)
            rs[d][slot].wait_recv()
            total = total + inbox[d, slot].astype(jnp.float32)
        for n in range(near):
            total_ref[:, features(quarter, n)] = total[:, n * block : (n + 1) * block]

    for copies in (*xs, *ys, *rs, own, *across):
        for copy in copies:
            copy.wait_send()


def finish(total_ref, wu, wd, post_hbm, mixed_hbm, up_hbm, down_hbm, mixed, post, sem):
    load = pltpu.make_async_copy(post_hbm, post, sem.at[3])
    load.start()
    copies = [
        pltpu.make_async_copy(src, dst, sem.at[k])
        for k, (src, dst) in enumerate(((wu, up_hbm), (wd, down_hbm), (mixed, mixed_hbm)))
    ]
    copies[0].start()
    copies[1].start()
    total = total_ref[...]
    scale = lax.rsqrt(jnp.mean(total * total, axis=1, keepdims=True) + EPS)
    load.wait()
    mixed[...] = (total * scale * post[...]).astype(jnp.bfloat16)
    copies[2].start()
    for copy in copies:
        copy.wait()


def solution(mesh):
    n_tp, n_fs = mesh.shape["tp"], mesh.shape["fs"]

    def per_device(*arrays):
        prompt_tokens, up_weight, down_weight, pre_gain, post_gain = (
            pltpu.with_memory_space_constraint(a[None, :] if a.ndim == 1 else a, pltpu.HBM) for a in arrays
        )
        rows, width = prompt_tokens.shape
        shard, units = up_weight.shape
        x_steps, y_steps = len(far_first(n_tp)), len(zero_and_two_first(n_fs // 2))
        vmem = pl.BlockSpec(memory_space=pltpu.VMEM)
        hbm = pl.BlockSpec(memory_space=pltpu.HBM)
        dma = pltpu.SemaphoreType.DMA
        total, sampler_up, sampler_down = pl.pallas_call(
            functools.partial(kernel, n_tp, n_fs),
            out_shape=(
                pltpu.VMEM((rows, width), jnp.float32),
                pltpu.VMEM((n_fs * shard, units), jnp.bfloat16),
                pltpu.VMEM((n_fs * shard, units), jnp.bfloat16),
            ),
            in_specs=[hbm, hbm, hbm, hbm],
            out_specs=(vmem, vmem, vmem),
            scratch_shapes=[
                pltpu.VMEM((rows, width), jnp.bfloat16),
                pltpu.VMEM((shard, units), jnp.float32),
                pltpu.VMEM((shard, units), jnp.float32),
                pltpu.VMEM((1, shard), jnp.float32),
                pltpu.VMEM((n_tp // 2, 2 * rows, width), jnp.bfloat16),
                pltpu.VMEM((n_tp // 2, 2 * rows, units), jnp.bfloat16),
                pltpu.VMEM((n_tp // 2, 2 * rows, width), jnp.float32),
                pltpu.VMEM((2, x_steps, rows, width // 4), jnp.bfloat16),
                pltpu.VMEM((2, x_steps, rows, width // 4), jnp.bfloat16),
                dma((4,)),
                dma((2, x_steps)),
                dma((2, x_steps)),
                dma((2, y_steps)),
                dma((2, y_steps)),
                dma((2 + 2 * y_steps,)),
                dma((2 + 2 * y_steps,)),
                dma((2, x_steps)),
                dma((2, x_steps)),
                pltpu.SemaphoreType.REGULAR((3,)),
            ],
            compiler_params=pltpu.CompilerParams(
                collective_id=0, has_side_effects=True, vmem_limit_bytes=42 * 2**20
            ),
        )(prompt_tokens, up_weight, down_weight, pre_gain)
        return pl.pallas_call(
            finish,
            out_shape=(
                jax.ShapeDtypeStruct((rows, width), jnp.bfloat16),
                jax.ShapeDtypeStruct((n_fs * shard, units), jnp.bfloat16),
                jax.ShapeDtypeStruct((n_fs * shard, units), jnp.bfloat16),
            ),
            in_specs=[vmem, vmem, vmem, hbm],
            out_specs=(hbm, hbm, hbm),
            scratch_shapes=[
                pltpu.VMEM((rows, width), jnp.bfloat16),
                pltpu.VMEM((1, width), jnp.float32),
                dma((4,)),
            ],
            compiler_params=pltpu.CompilerParams(vmem_limit_bytes=16 * 2**20),
        )(total, sampler_up, sampler_down, post_gain)

    placed = (P(("grp", "fs", "tp"), None), P("fs", "tp"), P("fs", "tp"), P("fs"), P())
    return jax.shard_map(
        per_device,
        mesh=mesh,
        in_specs=placed,
        out_specs=(P(("grp", "fs", "tp"), None), P("grp", "tp"), P("grp", "tp")),
        check_vma=False,
    )
```
